32 devices in a mesh: rep: 4 (over z), fs: 4 (over y, x), tp: 2 (over core).
Axes of the slice: x: 2, y: 2, z: 4, core: 2. Of those that a mesh axis runs over, the one named last changes fastest.
Arguments:
- inputs: bfloat16 [2048, 2048], P('rep', 'fs'), may hold values from -6 to 6
- w_gate: bfloat16 [2048, 3072], P('fs', 'tp'), may hold values from -0.125 to 0.125
- w_up: bfloat16 [2048, 3072], P('fs', 'tp'), may hold values from -0.125 to 0.125
- conv_taps: bfloat16 [3, 3072], P(None, 'tp'), may hold values from -3.5 to 3.5
- w_down: bfloat16 [3072, 2048], P('tp', 'fs'), may hold values from -0.109375 to 0.109375
- out_grad: bfloat16 [2048, 2048], P('rep', 'fs'), may hold values from -6 to 6
Outputs:
- in_grad: bfloat16 [2048, 2048], P(('rep', 'tp'), 'fs')
- grad_gate: float32 [2048, 3072], P('fs', 'tp')
- grad_up: float32 [2048, 3072], P('fs', 'tp')
- grad_down: float32 [3072, 2048], P('tp', 'fs')
- grad_taps: float32 [3, 3072], P(None, 'tp')
- rows_gate: float32 [2048], P('fs')
- rows_up: float32 [2048], P('fs')
- rows_down: float32 [3072], P('tp')
The draws below stay inside these ranges and needn't reach their ends.
All inputs are finite; a program needn't handle non-finite values.
Results may differ from the reference program's by a relative error of at most 0.025.
Values may be sent and summed in bfloat16 or wider, within the bound.
A program may use at most 64 MiB of HBM per device.

```python
import jax
import jax.numpy as jnp
from jax import lax

D = 2048
FF = 3072
KW = 3
TOK = 512
TOKENS = 2048
N_REP = 4
N_FS = 4
N_TP = 2


def with_spikes(values, rng, source, target, shards_of, factor):
    owner, partner = [(jnp.arange(values.shape[dim]) // (values.shape[dim] // shards_of)).reshape([-1 if axis == dim else 1 for axis in range(values.ndim)]) for dim in (source, target)]
    chosen = jax.random.permutation(rng, shards_of)[partner]
    strong = (owner == chosen) | (owner == (partner + shards_of // 2) % shards_of)
    return jnp.where(strong, factor * values, values)


def levels(key, shape, split, low, high):
    def one(axis_at, blocks):
        draws = jax.random.uniform(jax.random.fold_in(jax.random.fold_in(key, 6), axis_at), (blocks,), jnp.float32, low / len(split), high / len(split))
        return jnp.repeat(jnp.exp(draws), shape[axis_at] // blocks).reshape((-1,) + (1,) * (len(shape) - axis_at - 1))

    level = one(*split[0])
    for cut in split[1:]:
        level = level * one(*cut)
    return level


def bell_draw(stream_key, extent, spread, most, pieces=(), kind=jnp.bfloat16):
    entries = jax.random.normal(stream_key, extent, jnp.float32) * spread
    if len(pieces) > 0:
        entries = levels(stream_key, extent, pieces, -0.22, 0.18) * entries
    return jnp.clip(entries, min=-most, max=most).astype(kind)


def noise_with(stream_key, shape, scale, reach, pieces, heavy, dtype=jnp.bfloat16):
    entries = scale * jax.random.normal(stream_key, shape, jnp.float32)
    if pieces:
        entries = entries * levels(stream_key, shape, pieces, -0.22, 0.18)
    return jnp.clip(with_spikes(entries, jax.random.fold_in(stream_key, 3), *heavy), -reach, reach).astype(dtype)


def setup_inputs(seed: int = 0) -> dict:
    streams_of = jax.random.split(jax.random.key(seed), 7)
    inputs = bell_draw(streams_of[0], (TOKENS, D), 1.0, 6.0, ((0, 4), (1, 4)))
    w_gate = bell_draw(streams_of[1], (D, FF), D ** -0.5, 0.125, ((0, 4), (1, 2)))
    w_up = bell_draw(streams_of[2], (D, FF), D ** -0.5, 0.125, ((0, 4), (1, 2)))
    conv_taps = bell_draw(streams_of[3], (KW, FF), KW ** -0.5, 3.5, ((1, 2),))
    w_down = bell_draw(streams_of[4], (FF, D), FF ** -0.5, 0.109375, ((0, 2), (1, 4)))
    out_grad = noise_with(streams_of[5], (TOKENS, D), 1.0, 6.0, ((0, 4), (1, 4)), (0, 1, 4, 2.0))
    return {"inputs": inputs, "w_gate": w_gate, "w_up": w_up, "conv_taps": conv_taps, "w_down": w_down, "out_grad": out_grad}


def rounded(values):
    return lax.optimization_barrier(values.astype(jnp.bfloat16)).astype(jnp.float32)


def shift_down(values, lag_rows):
    if lag_rows == 0:
        return values
    padding = jnp.zeros_like(values[:, :lag_rows])
    return jnp.concatenate([padding, values[:, :-lag_rows]], axis=1)


def shift_up(values, lag_rows):
    if lag_rows == 0:
        return values
    padding = jnp.zeros_like(values[:, :lag_rows])
    return jnp.concatenate([values[:, lag_rows:], padding], axis=1)


def contract(left, right, left_dim, right_dim):
    return lax.dot_general(left, right, (((left_dim,), (right_dim,)), ((), ())), preferred_element_type=jnp.float32)


def reference(inputs, w_gate, w_up, conv_taps, w_down, out_grad):
    block_width = D // N_FS
    hidden_block = FF // N_TP
    gate_sum = jnp.zeros((TOKENS, FF), jnp.float32)
    up_sum = jnp.zeros((TOKENS, FF), jnp.float32)
    act_sum = jnp.zeros((TOKENS, FF), jnp.float32)
    for block_id in range(N_FS):
        start_col = block_id * block_width
        end_col = start_col + block_width
        gate_sum = gate_sum + rounded(jnp.dot(inputs[:, start_col:end_col], w_gate[start_col:end_col], preferred_element_type=jnp.float32))
        up_sum = up_sum + rounded(jnp.dot(inputs[:, start_col:end_col], w_up[start_col:end_col], preferred_element_type=jnp.float32))
        act_sum = act_sum + rounded(contract(out_grad[:, start_col:end_col], w_down[:, start_col:end_col], 1, 1))
    gate_pre = gate_sum.astype(jnp.bfloat16)
    up_val = up_sum.astype(jnp.bfloat16)
    act_grad = act_sum.astype(jnp.bfloat16)
    tap_weights = conv_taps.astype(jnp.float32)
    gate_seq = gate_pre.astype(jnp.float32).reshape(N_REP, TOK, FF)
    up_seq = up_val.astype(jnp.float32).reshape(N_REP, TOK, FF)
    act_seq = act_grad.astype(jnp.float32).reshape(N_REP, TOK, FF)
    pre_act = jnp.zeros((N_REP, TOK, FF), jnp.float32)
    for tap_index in range(KW):
        pre_act = pre_act + tap_weights[tap_index] * shift_down(gate_seq, KW - 1 - tap_index)
    sigmoid_pre = jax.nn.sigmoid(pre_act)
    hidden = (pre_act * sigmoid_pre * up_seq).astype(jnp.bfloat16)
    up_grad = (act_seq * pre_act * sigmoid_pre).astype(jnp.bfloat16)
    pre_grad = act_seq * up_seq * sigmoid_pre * (1.0 + pre_act * (1.0 - sigmoid_pre))
    gate_grad = jnp.zeros((N_REP, TOK, FF), jnp.float32)
    tap_list = []
    for tap_index in range(KW):
        gate_grad = gate_grad + tap_weights[tap_index] * shift_up(pre_grad, KW - 1 - tap_index)
        tap_list.append(jnp.sum(shift_down(gate_seq, KW - 1 - tap_index) * pre_grad, axis=(0, 1)))
    grad_taps = jnp.stack(tap_list)
    gate_grad = gate_grad.astype(jnp.bfloat16).reshape(TOKENS, FF)
    up_grad = up_grad.reshape(TOKENS, FF)
    hidden = hidden.reshape(TOKENS, FF)
    input_sum = jnp.zeros((TOKENS, D), jnp.float32)
    for block_id in range(N_TP):
        start_col = block_id * hidden_block
        end_col = start_col + hidden_block
        term = contract(gate_grad[:, start_col:end_col], w_gate[:, start_col:end_col], 1, 1)
        term = term + contract(up_grad[:, start_col:end_col], w_up[:, start_col:end_col], 1, 1)
        input_sum = input_sum + rounded(term)
    in_grad = input_sum.astype(jnp.bfloat16)
    grad_gate = contract(inputs, gate_grad, 0, 0)
    grad_up = contract(inputs, up_grad, 0, 0)
    grad_down = contract(hidden, out_grad, 0, 0)
    rows_gate = jnp.sum(grad_gate * grad_gate, axis=1)
    rows_up = jnp.sum(grad_up * grad_up, axis=1)
    rows_down = jnp.sum(grad_down * grad_down, axis=1)
    return (in_grad, grad_gate, grad_up, grad_down, grad_taps, rows_gate, rows_up, rows_down)
```

```python
import functools

import jax
import jax.numpy as jnp
from jax import lax
from jax.experimental import pallas as pl
from jax.experimental.pallas import tpu as pltpu
from jax.sharding import PartitionSpec as P

KW = 3


def shift_down(values, lag_rows):
    if lag_rows == 0:
        return values
    padding = jnp.zeros_like(values[:lag_rows])
    return jnp.concatenate([padding, values[:-lag_rows]], axis=0)


def shift_up(values, lag_rows):
    if lag_rows == 0:
        return values
    padding = jnp.zeros_like(values[:lag_rows])
    return jnp.concatenate([values[lag_rows:], padding], axis=0)


def contract(left, right, left_dim, right_dim):
    return lax.dot_general(
        left, right, (((left_dim,), (right_dim,)), ((), ())), preferred_element_type=jnp.float32
    )


def row_norms(grad_gate, grad_up, grad_down):
    gate_rows = jnp.sum(grad_gate * grad_gate, axis=1)
    up_rows = jnp.sum(grad_up * grad_up, axis=1)
    down_rows = jnp.sum(grad_down * grad_down, axis=1)
    gate_rows, up_rows = lax.psum((gate_rows, up_rows), "tp")
    down_rows = lax.psum(down_rows, "fs")
    return (gate_rows, up_rows, down_rows)


def shards(inputs, w_gate, w_up, conv_taps, w_down, out_grad):
    tap_weights = conv_taps.astype(jnp.float32)
    gate_part = jnp.dot(inputs, w_gate, preferred_element_type=jnp.float32)
    up_part = jnp.dot(inputs, w_up, preferred_element_type=jnp.float32)
    act_part = contract(out_grad, w_down, 1, 1)
    gate_sum, up_sum, act_sum = (
        lax.psum(gate_part.astype(jnp.bfloat16), "fs").astype(jnp.float32),
        lax.psum(up_part.astype(jnp.bfloat16), "fs").astype(jnp.float32),
        lax.psum(act_part.astype(jnp.bfloat16), "fs").astype(jnp.float32),
    )
    gate_pre = gate_sum.astype(jnp.bfloat16)
    up_val = up_sum.astype(jnp.bfloat16)
    act_grad = act_sum.astype(jnp.bfloat16)
    gate_float = gate_pre.astype(jnp.float32)
    up_float = up_val.astype(jnp.float32)
    act_float = act_grad.astype(jnp.float32)
    shifted = [shift_down(gate_float, KW - 1 - tap_index) for tap_index in range(KW)]
    pre_act = tap_weights[0] * shifted[0]
    for tap_index in range(1, KW):
        pre_act = pre_act + tap_weights[tap_index] * shifted[tap_index]
    sigmoid_pre = jax.nn.sigmoid(pre_act)
    hidden = (pre_act * sigmoid_pre * up_float).astype(jnp.bfloat16)
    up_grad = (act_float * pre_act * sigmoid_pre).astype(jnp.bfloat16)
    pre_grad = act_float * up_float * sigmoid_pre * (1.0 + pre_act * (1.0 - sigmoid_pre))
    gate_acc = tap_weights[0] * shift_up(pre_grad, KW - 1)
    for tap_index in range(1, KW):
        gate_acc = gate_acc + tap_weights[tap_index] * shift_up(pre_grad, KW - 1 - tap_index)
    gate_grad = gate_acc.astype(jnp.bfloat16)
    gate_rows = gate_grad
    up_rows = up_grad
    in_grad = lax.psum_scatter(
        (contract(gate_rows, w_gate, 1, 1) + contract(up_rows, w_up, 1, 1)).astype(jnp.bfloat16),
        "tp",
        scatter_dimension=0,
        tiled=True,
    )
    grad_gate = contract(inputs, gate_grad, 0, 0)
    grad_up = contract(inputs, up_grad, 0, 0)
    grad_down = contract(hidden, out_grad, 0, 0)
    grad_taps = jnp.stack(
        [jnp.sum(shifted[tap_index] * pre_grad, axis=0) for tap_index in range(KW)]
    )
    grad_gate, grad_up, grad_down, grad_taps = (
        lax.psum(grad_gate.astype(jnp.bfloat16), "rep").astype(jnp.float32),
        lax.psum(grad_up.astype(jnp.bfloat16), "rep").astype(jnp.float32),
        lax.psum(grad_down.astype(jnp.bfloat16), "rep").astype(jnp.float32),
        lax.psum(grad_taps.astype(jnp.bfloat16), "rep").astype(jnp.float32),
    )
    gate_rows, up_rows, down_rows = row_norms(grad_gate, grad_up, grad_down)
    weight_grads = (grad_gate, grad_up, grad_down, grad_taps, gate_rows, up_rows, down_rows)
    grad_gate, grad_up, grad_down, grad_taps, gate_rows, up_rows, down_rows = weight_grads
    return (in_grad, grad_gate, grad_up, grad_down, grad_taps, gate_rows, up_rows, down_rows)


LANES = 128
MID_LAG = 3
OUT_LAG = 8
MESH_ID = pl.DeviceIdType.MESH


def layer_kernel(
    n_rep, n_fs,
    x_ref, wg_ref, wu_ref, taps_ref, wd_ref, og_ref,
    in_grad_ref, pieces_ref, taps_out_ref, rows_gu_ref, rows_down_ref,
    xt, send_part, recv_part, h_all, g_all, u_all, part, from_out, from_in, tot,
    acc, ig_send, ig_recv, tap_all, tap_out, tap_in, rows, rows_tp, rows_fs,
    rs_send, rs_recv, ag_send, ag_recv, a_send, out_recv, in_recv, b_send, loc_sem, misc,
):
    tok, feat = x_ref.shape
    cw = n_fs * LANES
    chunks = wg_ref.shape[1] // cw
    subs = n_fs
    total_pieces = chunks * 3 * subs
    f32, bf16 = jnp.float32, jnp.bfloat16
    r = lax.axis_index("rep")
    f = lax.axis_index("fs")
    t = lax.axis_index("tp")
    half_rep = n_rep // 2
    is_left = r < half_rep
    toward = jnp.where(is_left, r + 1, r - 1)
    outward = jnp.where(is_left, r - 1, r + 1)
    is_end = jnp.logical_or(r == 0, r == n_rep - 1)
    not_end = jnp.logical_not(is_end)
    is_mid = jnp.logical_or(r == half_rep - 1, r == half_rep)
    not_mid = jnp.logical_not(is_mid)
    peers = [lax.rem(f + k, n_fs) for k in range(1, n_fs)]
    own_cols = pl.ds(pl.multiple_of(f * LANES, LANES), LANES)

    barrier = pltpu.get_barrier_semaphore()
    for k in range(n_fs - 1):
        pl.semaphore_signal(barrier, inc=1, device_id={"fs": peers[k]}, device_id_type=MESH_ID)
    pl.semaphore_signal(barrier, inc=1, device_id={"tp": 1 - t}, device_id_type=MESH_ID)
    pl.semaphore_signal(barrier, inc=1, device_id={"rep": toward}, device_id_type=MESH_ID)

    @pl.when(not_end)
    def _():
        pl.semaphore_signal(barrier, inc=1, device_id={"rep": outward}, device_id_type=MESH_ID)

    pl.semaphore_wait(barrier, n_fs + 1 + jnp.where(not_end, 1, 0))

    def remote(src, dst, send, recv, device):
        return pltpu.make_async_remote_copy(
            src_ref=src, dst_ref=dst, send_sem=send, recv_sem=recv,
            device_id=device, device_id_type=MESH_ID,
        )

    sent = []

    def rs_copy(c, tensor, k):
        s = (c * 3 + tensor) * (n_fs - 1) + k
        return remote(
            send_part.at[c, tensor, peers[k]], recv_part.at[c, tensor, k],
            rs_send.at[s], rs_recv.at[s], {"fs": peers[k]},
        )

    def reduce_start(c):
        cols = slice(c * cw, (c + 1) * cw)
        for tensor in range(3):
            if tensor == 0:
                value = jnp.dot(x_ref[...], wg_ref[:, cols], preferred_element_type=f32)
            elif tensor == 1:
                value = jnp.dot(x_ref[...], wu_ref[:, cols], preferred_element_type=f32)
            else:
                value = contract(og_ref[...], wd_ref[cols, :], 1, 1)
            value = value.astype(bf16)
            for g in range(n_fs):
                send_part[c, tensor, g] = value[:, g * LANES : (g + 1) * LANES]
            for k in range(n_fs - 1):
                copy = rs_copy(c, tensor, k)
                copy.start()
                sent.append(copy)

    def reduced(c, tensor):
        value = send_part[c, tensor, f].astype(f32)
        for k in range(n_fs - 1):
            rs_copy(c, tensor, k).wait_recv()
            value = value + recv_part[c, tensor, k].astype(f32)
        return value.astype(bf16).astype(f32)

    def ag_copy(c, tensor, k):
        s = (c * 3 + tensor) * (n_fs - 1) + k
        if tensor == 0:
            ref = h_all.at[c, f]
        elif tensor == 1:
            ref = g_all.at[c, :, own_cols]
        else:
            ref = u_all.at[c, :, own_cols]
        return remote(ref, ref, ag_send.at[s], ag_recv.at[s], {"fs": peers[k]})

    def gather_start(c, tensor):
        for k in range(n_fs - 1):
            copy = ag_copy(c, tensor, k)
            copy.start()
            sent.append(copy)

    row_ids = lax.broadcasted_iota(jnp.int32, (tok, LANES), 0)

    def down(value, lag):
        if lag == 0:
            return value
        return jnp.where(row_ids >= lag, pltpu.roll(value, lag, 0), 0.0)

    def up(value, lag):
        if lag == 0:
            return value
        return jnp.where(row_ids < tok - lag, pltpu.roll(value, tok - lag, 0), 0.0)

    def elementwise(c):
        cols = pl.ds(pl.multiple_of(c * cw + f * LANES, LANES), LANES)
        weights = taps_ref[:, cols].astype(f32)
        gate = reduced(c, 0)
        pre = weights[0:1] * down(gate, KW - 1)
        for j in range(1, KW):
            pre = pre + weights[j : j + 1] * down(gate, KW - 1 - j)
        sig = 1.0 / (1.0 + jnp.exp(-pre))
        silu = pre * sig
        up_val = reduced(c, 1)
        h_all[c, f] = (silu * up_val).T.astype(bf16)
        gather_start(c, 0)
        act = reduced(c, 2)
        pre_grad = act * up_val * sig * (1.0 + pre * (1.0 - sig))
        grad = weights[0:1] * up(pre_grad, KW - 1)
        for j in range(1, KW):
            grad = grad + weights[j : j + 1] * up(pre_grad, KW - 1 - j)
        g_all[c, :, own_cols] = grad.astype(bf16)
        gather_start(c, 1)
        u_all[c, :, own_cols] = (act * silu).astype(bf16)
        gather_start(c, 2)
        for j in range(KW):
            tap_all[f, c * 8 + j : c * 8 + j + 1, :] = jnp.sum(
                down(gate, KW - 1 - j) * pre_grad, axis=0, keepdims=True
            )

    def part_copy(p):
        return remote(part.at[p], from_out.at[p], a_send.at[p], out_recv.at[p], {"rep": toward})

    def exchange_copy(p):
        return remote(part.at[p], from_in.at[p], a_send.at[p], in_recv.at[p], {"rep": toward})

    def total_copy(p, src):
        return remote(src.at[p], from_in.at[p], b_send.at[p], in_recv.at[p], {"rep": outward})

    def local_copy(p, src):
        return pltpu.make_async_copy(src.at[p], pieces_ref.at[p], loc_sem.at[p])

    def stage_a(p, value):
        @pl.when(not_end)
        def _():
            part_copy(p).wait_recv()
            part[p] = (value + from_out[p].astype(f32)).astype(bf16)

        @pl.when(is_end)
        def _():
            part[p] = value.astype(bf16)

        @pl.when(is_mid)
        def _():
            exchange_copy(p).start()

        @pl.when(not_mid)
        def _():
            part_copy(p).start()

    def norms(p, value):
        square = value * value
        lanes = square[:, :LANES]
        for g in range(1, square.shape[1] // LANES):
            lanes = lanes + square[:, g * LANES : (g + 1) * LANES]
        rows[pl.ds(p, 1), :] = jnp.sum(lanes.T, axis=0, keepdims=True)

    def stage_b_mid(p):
        exchange_copy(p).wait_recv()
        value = (part[p].astype(f32) + from_in[p].astype(f32)).astype(bf16)
        tot[p] = value

        @pl.when(not_end)
        def _():
            total_copy(p, tot).start()

        local_copy(p, tot).start()
        norms(p, value.astype(f32))

    def stage_b_out(p):
        exchange_copy(p).wait_recv()

        @pl.when(not_end)
        def _():
            total_copy(p, from_in).start()

        local_copy(p, from_in).start()
        norms(p, from_in[p].astype(f32))

    def stage_b(slot):
        @pl.when(jnp.logical_and(is_mid, jnp.logical_and(slot >= MID_LAG, slot < total_pieces + MID_LAG)))
        def _():
            stage_b_mid(slot - MID_LAG)

        @pl.when(jnp.logical_and(not_mid, slot >= OUT_LAG))
        def _():
            stage_b_out(slot - OUT_LAG)

    def segment(c, tensor):
        for k in range(n_fs - 1):
            ag_copy(c, tensor, k).wait_recv()

        @pl.loop(0, subs)
        def _(q):
            p = (c * 3 + tensor) * subs + q
            if tensor == 0:
                value = jnp.dot(h_all[c, q], og_ref[...], preferred_element_type=f32)
            elif tensor == 1:
                value = jnp.dot(xt[q], g_all[c], preferred_element_type=f32)
            else:
                value = jnp.dot(xt[q], u_all[c], preferred_element_type=f32)
            stage_a(p, value)
            stage_b(p)

    def input_term(c):
        cols = slice(c * cw, (c + 1) * cw)
        term = contract(g_all[c], wg_ref[:, cols], 1, 1) + contract(u_all[c], wu_ref[:, cols], 1, 1)
        if c == 0:
            acc[...] = term
        else:
            acc[...] += term

    tap_all[...] = jnp.zeros_like(tap_all)
    reduce_start(0)
    for q in range(feat // LANES):
        xt[q] = x_ref[:, q * LANES : (q + 1) * LANES].astype(f32).T.astype(bf16)
    elementwise(0)
    if chunks > 1:
        reduce_start(1)
    tap_peers = []
    for c in range(chunks):
        segment(c, 0)
        segment(c, 1)
        if c + 1 < chunks:
            elementwise(c + 1)
            if c + 2 < chunks:
                reduce_start(c + 2)
        else:
            for k in range(n_fs - 1):
                copy = remote(
                    tap_all.at[f], tap_all.at[f], misc.at[2 * k], misc.at[2 * k + 1], {"fs": peers[k]}
                )
                copy.start()
                tap_peers.append(copy)
        segment(c, 2)
        input_term(c)

    m = 2 * (n_fs - 1)
    half = tok // 2
    ig_send[...] = acc[...].astype(bf16)
    ig_copy = remote(
        ig_send.at[pl.ds(pl.multiple_of((1 - t) * half, half), half)], ig_recv,
        misc.at[m], misc.at[m + 1], {"tp": 1 - t},
    )
    ig_copy.start()

    for copy in tap_peers:
        copy.wait()
    tap_part = remote(tap_all, tap_out, misc.at[m + 2], misc.at[m + 3], {"rep": toward})
    tap_exchange = remote(tap_all, tap_in, misc.at[m + 2], misc.at[m + 4], {"rep": toward})
    tap_total = remote(taps_out_ref, tap_in, misc.at[m + 5], misc.at[m + 4], {"rep": outward})

    @pl.when(not_end)
    def _():
        tap_part.wait_recv()
        tap_all[...] = tap_all[...] + tap_out[...]

    @pl.when(is_mid)
    def _():
        tap_exchange.start()

    @pl.when(not_mid)
    def _():
        tap_part.start()

    ig_copy.wait()
    in_grad_ref[...] = (
        ig_send[pl.ds(pl.multiple_of(t * half, half), half), :].astype(f32) + ig_recv[...].astype(f32)
    ).astype(bf16)

    @pl.loop(total_pieces, total_pieces + OUT_LAG)
    def _(slot):
        stage_b(slot)

    tap_exchange.wait_recv()

    @pl.when(is_mid)
    def _():
        taps_out_ref[...] = tap_all[...] + tap_in[...]

    @pl.when(not_mid)
    def _():
        taps_out_ref[...] = tap_in[...]

    @pl.when(not_end)
    def _():
        tap_total.start()

    rows_copies = [
        remote(rows, rows_tp, misc.at[m + 6], misc.at[m + 7], {"tp": 1 - t})
    ]
    for k in range(n_fs - 1):
        rows_copies.append(
            remote(rows, rows_fs.at[k], misc.at[m + 8 + 2 * k], misc.at[m + 9 + 2 * k], {"fs": peers[k]})
        )
    for copy in rows_copies:
        copy.start()

    for copy in sent:
        copy.wait_send()
    tap_part.wait_send()

    @pl.loop(0, total_pieces)
    def _(p):
        part_copy(p).wait_send()

        @pl.when(not_end)
        def _():
            total_copy(p, tot).wait_send()

        local_copy(p, tot).wait()

    for copy in rows_copies:
        copy.wait()
    for tensor in (1, 2):
        value = jnp.zeros((subs, LANES), f32)
        for c in range(chunks):
            at = (c * 3 + tensor) * subs
            value = value + (rows[at : at + subs, :] + rows_tp[at : at + subs, :])
        rows_gu_ref[(tensor - 1) * subs : tensor * subs, :] = value
    for c in range(chunks):
        at = c * 3 * subs
        value = rows[at : at + subs, :]
        for k in range(n_fs - 1):
            value = value + rows_fs[k, at : at + subs, :]
        rows_down_ref[c * subs : (c + 1) * subs, :] = value

    @pl.when(not_end)
    def _():
        tap_total.wait_send()


def fits(shape, inputs, w_gate):
    n_rep, n_fs, n_tp = shape["rep"], shape["fs"], shape["tp"]
    tok, feat = inputs.shape
    cw = n_fs * LANES
    return (
        n_rep == 4 and n_fs == 4 and n_tp == 2 and feat == cw
        and w_gate.shape[1] % cw == 0 and w_gate.shape[1] <= 1536 and tok % LANES == 0 and tok <= 512
    )


def fused_shards(shape, inputs, w_gate, w_up, conv_taps, w_down, out_grad):
    if not fits(shape, inputs, w_gate):
        return shards(inputs, w_gate, w_up, conv_taps, w_down, out_grad)
    n_rep, n_fs = shape["rep"], shape["fs"]
    tok, feat = inputs.shape
    hid = w_gate.shape[1]
    cw = n_fs * LANES
    chunks = hid // cw
    subs = n_fs
    pieces = chunks * 3 * subs
    bf16, f32 = jnp.bfloat16, jnp.float32
    vmem = pl.BlockSpec(memory_space=pltpu.VMEM)
    hops = chunks * 3 * (n_fs - 1)
    dma = pltpu.SemaphoreType.DMA
    in_grad, grads, taps, rows_gu, rows_down = pl.pallas_call(
        functools.partial(layer_kernel, n_rep, n_fs),
        out_shape=(
            jax.ShapeDtypeStruct((tok // 2, feat), bf16),
            jax.ShapeDtypeStruct((pieces, LANES, cw), bf16),
            jax.ShapeDtypeStruct((n_fs, chunks * 8, LANES), f32),
            jax.ShapeDtypeStruct((2 * subs, LANES), f32),
            jax.ShapeDtypeStruct((chunks * subs, LANES), f32),
        ),
        in_specs=[vmem] * 6,
        out_specs=(vmem, pl.BlockSpec(memory_space=pl.ANY), vmem, vmem, vmem),
        scratch_shapes=[
            pltpu.VMEM((subs, LANES, tok), bf16),
            pltpu.VMEM((chunks, 3, n_fs, tok, LANES), bf16),
            pltpu.VMEM((chunks, 3, n_fs - 1, tok, LANES), bf16),
            pltpu.VMEM((chunks, n_fs, LANES, tok), bf16),
            pltpu.VMEM((chunks, tok, cw), bf16),
            pltpu.VMEM((chunks, tok, cw), bf16),
            pltpu.VMEM((pieces, LANES, cw), bf16),
            pltpu.VMEM((pieces, LANES, cw), bf16),
            pltpu.VMEM((pieces, LANES, cw), bf16),
            pltpu.VMEM((pieces, LANES, cw), bf16),
            pltpu.VMEM((tok, feat), f32),
            pltpu.VMEM((tok, feat), bf16),
            pltpu.VMEM((tok // 2, feat), bf16),
            pltpu.VMEM((n_fs, chunks * 8, LANES), f32),
            pltpu.VMEM((n_fs, chunks * 8, LANES), f32),
            pltpu.VMEM((n_fs, chunks * 8, LANES), f32),
            pltpu.VMEM((pieces, LANES), f32),
            pltpu.VMEM((pieces, LANES), f32),
            pltpu.VMEM((n_fs - 1, pieces, LANES), f32),
            dma((hops,)), dma((hops,)), dma((hops,)), dma((hops,)),
            dma((pieces,)), dma((pieces,)), dma((pieces,)), dma((pieces,)), dma((pieces,)),
            dma((4 * (n_fs - 1) + 8,)),
        ],
        compiler_params=pltpu.CompilerParams(
            collective_id=0, has_side_effects=True, vmem_limit_bytes=60 * 1024 * 1024
        ),
    )(inputs, w_gate, w_up, conv_taps, w_down, out_grad)
    grads = grads.reshape(chunks, 3, subs, LANES, cw)
    grad_down = grads[:, 0].reshape(hid, feat).astype(f32)
    grad_gate = grads[:, 1].transpose(1, 2, 0, 3).reshape(feat, hid).astype(f32)
    grad_up = grads[:, 2].transpose(1, 2, 0, 3).reshape(feat, hid).astype(f32)
    grad_taps = taps.reshape(n_fs, chunks, 8, LANES)[:, :, :KW].transpose(2, 1, 0, 3).reshape(KW, hid)
    return (
        in_grad, grad_gate, grad_up, grad_down, grad_taps,
        rows_gu[:subs].reshape(feat), rows_gu[subs:].reshape(feat), rows_down.reshape(hid),
    )


def solution(mesh):
    return jax.shard_map(
        functools.partial(fused_shards, dict(mesh.shape)),
        mesh=mesh,
        in_specs=(
            P("rep", "fs"),
            P("fs", "tp"),
            P("fs", "tp"),
            P(None, "tp"),
            P("tp", "fs"),
            P("rep", "fs"),
        ),
        out_specs=(
            P(("rep", "tp"), "fs"),
            P("fs", "tp"),
            P("fs", "tp"),
            P("tp", "fs"),
            P(None, "tp"),
            P("fs"),
            P("fs"),
            P("tp"),
        ),
        check_vma=False,
    )
```

```python
import functools

import jax
import jax.numpy as jnp
from jax import lax
from jax.experimental import pallas as pl
from jax.experimental.pallas import tpu as pltpu
from jax.sharding import PartitionSpec as P

KW = 3


def shift_down(values, lag_rows):
    if lag_rows == 0:
        return values
    padding = jnp.zeros_like(values[:lag_rows])
    return jnp.concatenate([padding, values[:-lag_rows]], axis=0)


def shift_up(values, lag_rows):
    if lag_rows == 0:
        return values
    padding = jnp.zeros_like(values[:lag_rows])
    return jnp.concatenate([values[lag_rows:], padding], axis=0)


def contract(left, right, left_dim, right_dim):
    return lax.dot_general(
        left, right, (((left_dim,), (right_dim,)), ((), ())), preferred_element_type=jnp.float32
    )


def row_norms(grad_gate, grad_up, grad_down):
    gate_rows = jnp.sum(grad_gate * grad_gate, axis=1)
    up_rows = jnp.sum(grad_up * grad_up, axis=1)
    down_rows = jnp.sum(grad_down * grad_down, axis=1)
    gate_rows, up_rows = lax.psum((gate_rows, up_rows), "tp")
    down_rows = lax.psum(down_rows, "fs")
    return (gate_rows, up_rows, down_rows)


def shards(inputs, w_gate, w_up, conv_taps, w_down, out_grad):
    tap_weights = conv_taps.astype(jnp.float32)
    gate_part = jnp.dot(inputs, w_gate, preferred_element_type=jnp.float32)
    up_part = jnp.dot(inputs, w_up, preferred_element_type=jnp.float32)
    act_part = contract(out_grad, w_down, 1, 1)
    gate_sum, up_sum, act_sum = (
        lax.psum(gate_part.astype(jnp.bfloat16), "fs").astype(jnp.float32),
        lax.psum(up_part.astype(jnp.bfloat16), "fs").astype(jnp.float32),
        lax.psum(act_part.astype(jnp.bfloat16), "fs").astype(jnp.float32),
    )
    gate_pre = gate_sum.astype(jnp.bfloat16)
    up_val = up_sum.astype(jnp.bfloat16)
    act_grad = act_sum.astype(jnp.bfloat16)
    gate_float = gate_pre.astype(jnp.float32)
    up_float = up_val.astype(jnp.float32)
    act_float = act_grad.astype(jnp.float32)
    shifted = [shift_down(gate_float, KW - 1 - tap_index) for tap_index in range(KW)]
    pre_act = tap_weights[0] * shifted[0]
    for tap_index in range(1, KW):
        pre_act = pre_act + tap_weights[tap_index] * shifted[tap_index]
    sigmoid_pre = jax.nn.sigmoid(pre_act)
    hidden = (pre_act * sigmoid_pre * up_float).astype(jnp.bfloat16)
    up_grad = (act_float * pre_act * sigmoid_pre).astype(jnp.bfloat16)
    pre_grad = act_float * up_float * sigmoid_pre * (1.0 + pre_act * (1.0 - sigmoid_pre))
    gate_acc = tap_weights[0] * shift_up(pre_grad, KW - 1)
    for tap_index in range(1, KW):
        gate_acc = gate_acc + tap_weights[tap_index] * shift_up(pre_grad, KW - 1 - tap_index)
    gate_grad = gate_acc.astype(jnp.bfloat16)
    gate_rows = gate_grad
    up_rows = up_grad
    in_grad = lax.psum_scatter(
        (contract(gate_rows, w_gate, 1, 1) + contract(up_rows, w_up, 1, 1)).astype(jnp.bfloat16),
        "tp",
        scatter_dimension=0,
        tiled=True,
    )
    grad_gate = contract(inputs, gate_grad, 0, 0)
    grad_up = contract(inputs, up_grad, 0, 0)
    grad_down = contract(hidden, out_grad, 0, 0)
    grad_taps = jnp.stack(
        [jnp.sum(shifted[tap_index] * pre_grad, axis=0) for tap_index in range(KW)]
    )
    grad_gate, grad_up, grad_down, grad_taps = (
        lax.psum(grad_gate.astype(jnp.bfloat16), "rep").astype(jnp.float32),
        lax.psum(grad_up.astype(jnp.bfloat16), "rep").astype(jnp.float32),
        lax.psum(grad_down.astype(jnp.bfloat16), "rep").astype(jnp.float32),
        lax.psum(grad_taps.astype(jnp.bfloat16), "rep").astype(jnp.float32),
    )
    gate_rows, up_rows, down_rows = row_norms(grad_gate, grad_up, grad_down)
    weight_grads = (grad_gate, grad_up, grad_down, grad_taps, gate_rows, up_rows, down_rows)
    grad_gate, grad_up, grad_down, grad_taps, gate_rows, up_rows, down_rows = weight_grads
    return (in_grad, grad_gate, grad_up, grad_down, grad_taps, gate_rows, up_rows, down_rows)


LANES = 128
CW = 256
HALO = 16
MID_LAG = 3
OUT_LAG = 8
MESH_ID = pl.DeviceIdType.MESH


def layer_kernel(
    n_rep, n_fs,
    x_ref, wg_ref, wu_ref, taps_ref, wd_ref, og_ref,
    in_grad_ref, down_ref, gate_ref, up_ref, taps_out_ref, rows_gate_ref, rows_up_ref, rows_down_ref,
    xt, send_part, recv_part, h_all, g_all, u_all, part, from_out, from_in, tot,
    acc, ig_send, ig_recv, tap_all, tap_out, tap_in, tap_sum, rows, rows_tp, rows_fs,
    rs_send, rs_recv, ag_send, ag_recv, a_send, out_recv, in_recv, b_send, loc_sem, misc,
):
    tok, feat = x_ref.shape
    cw = CW
    chunks = wg_ref.shape[1] // cw
    subs = feat // cw
    own_rows = tok // 2
    span = own_rows + HALO
    total_pieces = chunks * 3 * subs
    f32, bf16 = jnp.float32, jnp.bfloat16
    r = lax.axis_index("rep")
    f = lax.axis_index("fs")
    t = lax.axis_index("tp")
    half_rep = n_rep // 2
    is_left = r < half_rep
    toward = jnp.where(is_left, r + 1, r - 1)
    outward = jnp.where(is_left, r - 1, r + 1)
    is_end = jnp.logical_or(r == 0, r == n_rep - 1)
    not_end = jnp.logical_not(is_end)
    is_mid = jnp.logical_or(r == half_rep - 1, r == half_rep)
    not_mid = jnp.logical_not(is_mid)
    beside = f + 1 - 2 * lax.rem(f, 2)
    across = lax.rem(f + 2, 4)
    corner = lax.rem(beside + 2, 4)
    peers = [beside, across, corner]
    side = lax.rem(f, 2)
    top = f // 2
    own_cols = pl.ds(pl.multiple_of(side * LANES, LANES), LANES)
    own_toks = pl.ds(pl.multiple_of(top * own_rows, own_rows), own_rows)

    barrier = pltpu.get_barrier_semaphore()
    for k in range(n_fs - 1):
        pl.semaphore_signal(barrier, inc=1, device_id={"fs": peers[k]}, device_id_type=MESH_ID)
    pl.semaphore_signal(barrier, inc=1, device_id={"tp": 1 - t}, device_id_type=MESH_ID)
    pl.semaphore_signal(barrier, inc=1, device_id={"rep": toward}, device_id_type=MESH_ID)

    @pl.when(not_end)
    def _():
        pl.semaphore_signal(barrier, inc=1, device_id={"rep": outward}, device_id_type=MESH_ID)

    pl.semaphore_wait(barrier, n_fs + 1 + jnp.where(not_end, 1, 0))

    def remote(src, dst, send, recv, device):
        return pltpu.make_async_remote_copy(
            src_ref=src, dst_ref=dst, send_sem=send, recv_sem=recv,
            device_id=device, device_id_type=MESH_ID,
        )

    sent = []

    def rs_copy(c, tensor, k):
        s = (c * 3 + tensor) * (n_fs - 1) + k
        return remote(
            send_part.at[c, tensor, peers[k]], recv_part.at[c, tensor, k],
            rs_send.at[s], rs_recv.at[s], {"fs": peers[k]},
        )

    def reduce_start(c):
        cols = slice(c * cw, (c + 1) * cw)
        for tensor in range(3):
            if tensor == 0:
                value = jnp.dot(x_ref[...], wg_ref[:, cols], preferred_element_type=f32)
            elif tensor == 1:
                value = jnp.dot(x_ref[...], wu_ref[:, cols], preferred_element_type=f32)
            else:
                value = contract(og_ref[...], wd_ref[cols, :], 1, 1)
            value = value.astype(bf16)
            for g in range(n_fs):
                first = (g // 2) * (own_rows - HALO)
                lane = (g % 2) * LANES
                send_part[c, tensor, g] = value[first : first + span, lane : lane + LANES]
            for k in range(n_fs - 1):
                copy = rs_copy(c, tensor, k)
                copy.start()
                sent.append(copy)

    def reduced(c, tensor):
        value = send_part[c, tensor, f].astype(f32)
        for k in range(n_fs - 1):
            rs_copy(c, tensor, k).wait_recv()
            value = value + recv_part[c, tensor, k].astype(f32)
        return value.astype(bf16).astype(f32)

    def block(c, tensor, owner, part_of=None):
        col = lax.rem(owner, 2) * LANES
        row = (owner // 2) * own_rows
        if tensor == 0:
            size = LANES if part_of is None else LANES // 2
            start = col + (0 if part_of is None else part_of * size)
            return h_all.at[
                c, pl.ds(pl.multiple_of(start, size), size), pl.ds(pl.multiple_of(row, own_rows), own_rows)
            ]
        size = own_rows if part_of is None else own_rows // 2
        start = row + (0 if part_of is None else part_of * size)
        ref = g_all if tensor == 1 else u_all
        return ref.at[c, pl.ds(pl.multiple_of(start, size), size), pl.ds(pl.multiple_of(col, LANES), LANES)]

    def ag_copy(c, tensor, step, owner):
        s = (c * 3 + tensor) * 4
        if step == 0:
            ref, slot, target = block(c, tensor, owner), 0, beside
        elif step == 1:
            ref, slot, target = block(c, tensor, owner), 1, across
        elif step == 2:
            ref, slot, target = block(c, tensor, owner, 1), 2, beside
        else:
            ref, slot, target = block(c, tensor, owner, 0), 3, across
        return remote(ref, ref, ag_send.at[s + slot], ag_recv.at[s + slot], {"fs": target})

    def gather_start(c, tensor):
        for step in (0, 1):
            copy = ag_copy(c, tensor, step, f)
            copy.start()
            sent.append(copy)

    def forward(c, tensor):
        ag_copy(c, tensor, 0, beside).wait_recv()
        copy = ag_copy(c, tensor, 3, beside)
        copy.start()
        sent.append(copy)
        ag_copy(c, tensor, 1, across).wait_recv()
        copy = ag_copy(c, tensor, 2, across)
        copy.start()
        sent.append(copy)

    def gathered(c, tensor):
        ag_copy(c, tensor, 2, corner).wait_recv()
        ag_copy(c, tensor, 3, corner).wait_recv()

    def own(value):
        return jnp.where(top == 0, value[:own_rows], value[HALO:])

    row_ids = lax.broadcasted_iota(jnp.int32, (span, LANES), 0)

    def down(value, lag):
        if lag == 0:
            return value
        return jnp.where(row_ids >= lag, pltpu.roll(value, lag, 0), 0.0)

    def up(value, lag):
        if lag == 0:
            return value
        return jnp.where(row_ids < span - lag, pltpu.roll(value, span - lag, 0), 0.0)

    def elementwise(c):
        cols = pl.ds(pl.multiple_of(c * cw + side * LANES, LANES), LANES)
        weights = taps_ref[:, cols].astype(f32)
        gate = reduced(c, 0)
        pre = weights[0:1] * down(gate, KW - 1)
        for j in range(1, KW):
            pre = pre + weights[j : j + 1] * down(gate, KW - 1 - j)
        sig = 1.0 / (1.0 + jnp.exp(-pre))
        silu = pre * sig
        up_val = reduced(c, 1)
        h_all[c, own_cols, own_toks] = own(silu * up_val).T.astype(bf16)
        gather_start(c, 0)
        act = reduced(c, 2)
        pre_grad = act * up_val * sig * (1.0 + pre * (1.0 - sig))
        grad = weights[0:1] * up(pre_grad, KW - 1)
        for j in range(1, KW):
            grad = grad + weights[j : j + 1] * up(pre_grad, KW - 1 - j)
        g_all[c, own_toks, own_cols] = own(grad).astype(bf16)
        gather_start(c, 1)
        u_all[c, own_toks, own_cols] = own(act * silu).astype(bf16)
        gather_start(c, 2)
        for j in range(KW):
            tap_all[f, c * KW + j : c * KW + j + 1, :] = jnp.sum(
                own(down(gate, KW - 1 - j) * pre_grad), axis=0, keepdims=True
            )

    def part_copy(p):
        return remote(part.at[p], from_out.at[p], a_send.at[p], out_recv.at[p], {"rep": toward})

    def exchange_copy(p):
        return remote(part.at[p], from_in.at[p], a_send.at[p], in_recv.at[p], {"rep": toward})

    def total_copy(p, src):
        return remote(src.at[p], from_in.at[p], b_send.at[p], in_recv.at[p], {"rep": outward})

    def local_copy(p, src, tensor, wait):
        c = p // (3 * subs)
        q = p % subs
        along = pl.ds(pl.multiple_of(c * cw, cw), cw)
        inner = pl.ds(pl.multiple_of(q * cw, cw), cw)
        if tensor == 0:
            dst = down_ref.at[along, inner]
        elif tensor == 1:
            dst = gate_ref.at[inner, along]
        else:
            dst = up_ref.at[inner, along]
        copy = pltpu.make_async_copy(src.at[p], dst, loc_sem.at[p])
        if wait:
            copy.wait()
        else:
            copy.start()

    def store_out(p, src, wait=False):
        kind = (p // subs) % 3
        for tensor in range(3):
            @pl.when(kind == tensor)
            def _(tensor=tensor):
                local_copy(p, src, tensor, wait)

    def stage_a(p, value):
        @pl.when(not_end)
        def _():
            part_copy(p).wait_recv()
            part[p] = (value + from_out[p].astype(f32)).astype(bf16)

        @pl.when(is_end)
        def _():
            part[p] = value.astype(bf16)

        @pl.when(is_mid)
        def _():
            exchange_copy(p).start()

        @pl.when(not_mid)
        def _():
            part_copy(p).start()

    def norms(p, value):
        square = value * value
        lanes = square[:, :LANES]
        for g in range(1, square.shape[1] // LANES):
            lanes = lanes + square[:, g * LANES : (g + 1) * LANES]
        for i in range(cw // LANES):
            rows[pl.ds(p * (cw // LANES) + i, 1), :] = jnp.sum(
                lanes[i * LANES : (i + 1) * LANES].T, axis=0, keepdims=True
            )

    def stage_b_mid(p):
        exchange_copy(p).wait_recv()
        value = (part[p].astype(f32) + from_in[p].astype(f32)).astype(bf16)
        tot[p] = value

        @pl.when(not_end)
        def _():
            total_copy(p, tot).start()

        store_out(p, tot)
        norms(p, value.astype(f32))

    def stage_b_out(p):
        exchange_copy(p).wait_recv()

        @pl.when(not_end)
        def _():
            total_copy(p, from_in).start()

        store_out(p, from_in)
        norms(p, from_in[p].astype(f32))

    def stage_b(slot):
        @pl.when(jnp.logical_and(is_mid, jnp.logical_and(slot >= MID_LAG, slot < total_pieces + MID_LAG)))
        def _():
            stage_b_mid(slot - MID_LAG)

        @pl.when(jnp.logical_and(not_mid, slot >= OUT_LAG))
        def _():
            stage_b_out(slot - OUT_LAG)

    def segment(c, tensor):
        gathered(c, tensor)

        @pl.loop(0, subs)
        def _(q):
            p = (c * 3 + tensor) * subs + q
            if tensor == 0:
                value = jnp.dot(
                    h_all[c], og_ref[:, pl.ds(pl.multiple_of(q * cw, cw), cw)], preferred_element_type=f32
                )
            elif tensor == 1:
                value = jnp.dot(xt[q], g_all[c], preferred_element_type=f32)
            else:
                value = jnp.dot(xt[q], u_all[c], preferred_element_type=f32)
            stage_a(p, value)
            stage_b(p)

    def input_term(c):
        cols = slice(c * cw, (c + 1) * cw)
        term = contract(g_all[c], wg_ref[:, cols], 1, 1) + contract(u_all[c], wu_ref[:, cols], 1, 1)
        if c == 0:
            acc[...] = term
        else:
            acc[...] += term

    reduce_start(0)
    for q in range(subs):
        xt[q] = x_ref[:, q * cw : (q + 1) * cw].astype(f32).T.astype(bf16)
    elementwise(0)
    if chunks > 1:
        reduce_start(1)
    tap_peers = []

    def advance(c):
        if c < chunks:
            elementwise(c)
            if c + 1 < chunks:
                reduce_start(c + 1)
        else:
            for k in range(n_fs - 1):
                copy = remote(
                    tap_all.at[f], tap_all.at[f], misc.at[2 * k], misc.at[2 * k + 1], {"fs": peers[k]}
                )
                copy.start()
                tap_peers.append(copy)

    forward(0, 0)
    for c in range(chunks):
        segment(c, 0)
        if c > 0:
            advance(c + 1)
        forward(c, 1)
        if c > 0:
            forward(c, 2)
        segment(c, 1)
        if c == 0:
            forward(c, 2)
            advance(c + 1)
        segment(c, 2)
        if c + 1 < chunks:
            forward(c + 1, 0)
        input_term(c)

    m = 2 * (n_fs - 1)
    half = tok // 2
    ig_send[...] = acc[...].astype(bf16)
    ig_copy = remote(
        ig_send.at[pl.ds(pl.multiple_of((1 - t) * half, half), half)], ig_recv,
        misc.at[m], misc.at[m + 1], {"tp": 1 - t},
    )
    ig_copy.start()

    for copy in tap_peers:
        copy.wait()
    tap_part = remote(tap_all, tap_out, misc.at[m + 2], misc.at[m + 3], {"rep": toward})
    tap_exchange = remote(tap_all, tap_in, misc.at[m + 2], misc.at[m + 4], {"rep": toward})
    tap_total = remote(tap_sum, tap_in, misc.at[m + 5], misc.at[m + 4], {"rep": outward})

    @pl.when(not_end)
    def _():
        tap_part.wait_recv()
        tap_all[...] = tap_all[...] + tap_out[...]

    @pl.when(is_mid)
    def _():
        tap_exchange.start()

    @pl.when(not_mid)
    def _():
        tap_part.start()

    ig_copy.wait()
    in_grad_ref[...] = (
        ig_send[pl.ds(pl.multiple_of(t * half, half), half), :].astype(f32) + ig_recv[...].astype(f32)
    ).astype(bf16)

    @pl.loop(total_pieces, total_pieces + OUT_LAG)
    def _(slot):
        stage_b(slot)

    tap_exchange.wait_recv()

    @pl.when(is_mid)
    def _():
        tap_sum[...] = tap_all[...] + tap_in[...]

    @pl.when(not_mid)
    def _():
        tap_sum[...] = tap_in[...]

    @pl.when(not_end)
    def _():
        tap_total.start()

    rows_copies = [
        remote(rows, rows_tp, misc.at[m + 6], misc.at[m + 7], {"tp": 1 - t})
    ]
    for k in range(n_fs - 1):
        rows_copies.append(
            remote(rows, rows_fs.at[k], misc.at[m + 8 + 2 * k], misc.at[m + 9 + 2 * k], {"fs": peers[k]})
        )
    for copy in rows_copies:
        copy.start()

    for copy in sent:
        copy.wait_send()
    tap_part.wait_send()

    @pl.loop(0, total_pieces)
    def _(p):
        part_copy(p).wait_send()

        @pl.when(not_end)
        def _():
            total_copy(p, tot).wait_send()

        store_out(p, tot, True)

    for copy in rows_copies:
        copy.wait()
    per = cw // LANES
    for tensor, rows_ref in ((1, rows_gate_ref), (2, rows_up_ref)):
        for q in range(subs):
            for i in range(per):
                value = jnp.zeros((1, LANES), f32)
                for c in range(chunks):
                    at = ((c * 3 + tensor) * subs + q) * per + i
                    value = value + (rows[at : at + 1, :] + rows_tp[at : at + 1, :])
                lane = (q * per + i) * LANES
                rows_ref[:, lane : lane + LANES] = value
    for c in range(chunks):
        for i in range(per):
            value = jnp.zeros((1, LANES), f32)
            for q in range(subs):
                at = (c * 3 * subs + q) * per + i
                value = value + rows[at : at + 1, :]
                for k in range(n_fs - 1):
                    value = value + rows_fs[k, at : at + 1, :]
            lane = (c * per + i) * LANES
            rows_down_ref[:, lane : lane + LANES] = value
            for j in range(KW):
                at = c * KW + j
                taps_out_ref[j : j + 1, lane : lane + LANES] = (
                    tap_sum[i, at : at + 1, :] + tap_sum[i + 2, at : at + 1, :]
                )

    @pl.when(not_end)
    def _():
        tap_total.wait_send()


def fits(shape, inputs, w_gate):
    n_rep, n_fs, n_tp = shape["rep"], shape["fs"], shape["tp"]
    tok, feat = inputs.shape
    return (
        n_rep == 4 and n_fs == 4 and n_tp == 2 and feat == 2 * CW
        and w_gate.shape[1] % CW == 0 and w_gate.shape[1] <= 1536 and tok % LANES == 0 and tok <= 512
    )


def fused_shards(shape, inputs, w_gate, w_up, conv_taps, w_down, out_grad):
    if not fits(shape, inputs, w_gate):
        return shards(inputs, w_gate, w_up, conv_taps, w_down, out_grad)
    n_rep, n_fs = shape["rep"], shape["fs"]
    tok, feat = inputs.shape
    hid = w_gate.shape[1]
    cw = CW
    chunks = hid // cw
    subs = feat // cw
    pieces = chunks * 3 * subs
    bf16, f32 = jnp.bfloat16, jnp.float32
    vmem = pl.BlockSpec(memory_space=pltpu.VMEM)
    hops = chunks * 3 * (n_fs - 1)
    dma = pltpu.SemaphoreType.DMA
    in_grad, down, gate, up, taps, rows_gate, rows_up, rows_down = pl.pallas_call(
        functools.partial(layer_kernel, n_rep, n_fs),
        out_shape=(
            jax.ShapeDtypeStruct((tok // 2, feat), bf16),
            jax.ShapeDtypeStruct((hid, feat), bf16),
            jax.ShapeDtypeStruct((feat, hid), bf16),
            jax.ShapeDtypeStruct((feat, hid), bf16),
            jax.ShapeDtypeStruct((KW, hid), f32),
            jax.ShapeDtypeStruct((1, feat), f32),
            jax.ShapeDtypeStruct((1, feat), f32),
            jax.ShapeDtypeStruct((1, hid), f32),
        ),
        in_specs=[vmem] * 6,
        out_specs=(vmem,) + (pl.BlockSpec(memory_space=pl.ANY),) * 3 + (vmem,) * 4,
        scratch_shapes=[
            pltpu.VMEM((subs, cw, tok), bf16),
            pltpu.VMEM((chunks, 3, n_fs, tok // 2 + HALO, LANES), bf16),
            pltpu.VMEM((chunks, 3, n_fs - 1, tok // 2 + HALO, LANES), bf16),
            pltpu.VMEM((chunks, cw, tok), bf16),
            pltpu.VMEM((chunks, tok, cw), bf16),
            pltpu.VMEM((chunks, tok, cw), bf16),
            pltpu.VMEM((pieces, cw, cw), bf16),
            pltpu.VMEM((pieces, cw, cw), bf16),
            pltpu.VMEM((pieces, cw, cw), bf16),
            pltpu.VMEM((pieces, cw, cw), bf16),
            pltpu.VMEM((tok, feat), f32),
            pltpu.VMEM((tok, feat), bf16),
            pltpu.VMEM((tok // 2, feat), bf16),
            pltpu.VMEM((n_fs, chunks * KW, LANES), f32),
            pltpu.VMEM((n_fs, chunks * KW, LANES), f32),
            pltpu.VMEM((n_fs, chunks * KW, LANES), f32),
            pltpu.VMEM((n_fs, chunks * KW, LANES), f32),
            pltpu.VMEM((2 * pieces, LANES), f32),
            pltpu.VMEM((2 * pieces, LANES), f32),
            pltpu.VMEM((n_fs - 1, 2 * pieces, LANES), f32),
            dma((hops,)), dma((hops,)), dma((chunks * 12,)), dma((chunks * 12,)),
            dma((pieces,)), dma((pieces,)), dma((pieces,)), dma((pieces,)), dma((pieces,)),
            dma((4 * (n_fs - 1) + 8,)),
        ],
        compiler_params=pltpu.CompilerParams(
            collective_id=0, has_side_effects=True, vmem_limit_bytes=60 * 1024 * 1024
        ),
    )(inputs, w_gate, w_up, conv_taps, w_down, out_grad)
    return (
        in_grad, gate.astype(f32), up.astype(f32), down.astype(f32), taps,
        rows_gate.reshape(feat), rows_up.reshape(feat), rows_down.reshape(hid),
    )


def solution(mesh):
    return jax.shard_map(
        functools.partial(fused_shards, dict(mesh.shape)),
        mesh=mesh,
        in_specs=(
            P("rep", "fs"),
            P("fs", "tp"),
            P("fs", "tp"),
            P(None, "tp"),
            P("tp", "fs"),
            P("rep", "fs"),
        ),
        out_specs=(
            P(("rep", "tp"), "fs"),
            P("fs", "tp"),
            P("fs", "tp"),
            P("tp", "fs"),
            P(None, "tp"),
            P("fs"),
            P("fs"),
            P("tp"),
        ),
        check_vma=False,
    )
```

```python
import functools

import jax
import jax.numpy as jnp
from jax import lax
from jax.experimental import pallas as pl
from jax.experimental.pallas import tpu as pltpu
from jax.sharding import PartitionSpec as P

KW = 3


def shift_down(values, lag_rows):
    if lag_rows == 0:
        return values
    padding = jnp.zeros_like(values[:lag_rows])
    return jnp.concatenate([padding, values[:-lag_rows]], axis=0)


def shift_up(values, lag_rows):
    if lag_rows == 0:
        return values
    padding = jnp.zeros_like(values[:lag_rows])
    return jnp.concatenate([values[lag_rows:], padding], axis=0)


def contract(left, right, left_dim, right_dim):
    return lax.dot_general(
        left, right, (((left_dim,), (right_dim,)), ((), ())), preferred_element_type=jnp.float32
    )


def row_norms(grad_gate, grad_up, grad_down):
    gate_rows = jnp.sum(grad_gate * grad_gate, axis=1)
    up_rows = jnp.sum(grad_up * grad_up, axis=1)
    down_rows = jnp.sum(grad_down * grad_down, axis=1)
    gate_rows, up_rows = lax.psum((gate_rows, up_rows), "tp")
    down_rows = lax.psum(down_rows, "fs")
    return (gate_rows, up_rows, down_rows)


def shards(inputs, w_gate, w_up, conv_taps, w_down, out_grad):
    tap_weights = conv_taps.astype(jnp.float32)
    gate_part = jnp.dot(inputs, w_gate, preferred_element_type=jnp.float32)
    up_part = jnp.dot(inputs, w_up, preferred_element_type=jnp.float32)
    act_part = contract(out_grad, w_down, 1, 1)
    gate_sum, up_sum, act_sum = (
        lax.psum(gate_part.astype(jnp.bfloat16), "fs").astype(jnp.float32),
        lax.psum(up_part.astype(jnp.bfloat16), "fs").astype(jnp.float32),
        lax.psum(act_part.astype(jnp.bfloat16), "fs").astype(jnp.float32),
    )
    gate_pre = gate_sum.astype(jnp.bfloat16)
    up_val = up_sum.astype(jnp.bfloat16)
    act_grad = act_sum.astype(jnp.bfloat16)
    gate_float = gate_pre.astype(jnp.float32)
    up_float = up_val.astype(jnp.float32)
    act_float = act_grad.astype(jnp.float32)
    shifted = [shift_down(gate_float, KW - 1 - tap_index) for tap_index in range(KW)]
    pre_act = tap_weights[0] * shifted[0]
    for tap_index in range(1, KW):
        pre_act = pre_act + tap_weights[tap_index] * shifted[tap_index]
    sigmoid_pre = jax.nn.sigmoid(pre_act)
    hidden = (pre_act * sigmoid_pre * up_float).astype(jnp.bfloat16)
    up_grad = (act_float * pre_act * sigmoid_pre).astype(jnp.bfloat16)
    pre_grad = act_float * up_float * sigmoid_pre * (1.0 + pre_act * (1.0 - sigmoid_pre))
    gate_acc = tap_weights[0] * shift_up(pre_grad, KW - 1)
    for tap_index in range(1, KW):
        gate_acc = gate_acc + tap_weights[tap_index] * shift_up(pre_grad, KW - 1 - tap_index)
    gate_grad = gate_acc.astype(jnp.bfloat16)
    gate_rows = gate_grad
    up_rows = up_grad
    in_grad = lax.psum_scatter(
        (contract(gate_rows, w_gate, 1, 1) + contract(up_rows, w_up, 1, 1)).astype(jnp.bfloat16),
        "tp",
        scatter_dimension=0,
        tiled=True,
    )
    grad_gate = contract(inputs, gate_grad, 0, 0)
    grad_up = contract(inputs, up_grad, 0, 0)
    grad_down = contract(hidden, out_grad, 0, 0)
    grad_taps = jnp.stack(
        [jnp.sum(shifted[tap_index] * pre_grad, axis=0) for tap_index in range(KW)]
    )
    grad_gate, grad_up, grad_down, grad_taps = (
        lax.psum(grad_gate.astype(jnp.bfloat16), "rep").astype(jnp.float32),
        lax.psum(grad_up.astype(jnp.bfloat16), "rep").astype(jnp.float32),
        lax.psum(grad_down.astype(jnp.bfloat16), "rep").astype(jnp.float32),
        lax.psum(grad_taps.astype(jnp.bfloat16), "rep").astype(jnp.float32),
    )
    gate_rows, up_rows, down_rows = row_norms(grad_gate, grad_up, grad_down)
    weight_grads = (grad_gate, grad_up, grad_down, grad_taps, gate_rows, up_rows, down_rows)
    grad_gate, grad_up, grad_down, grad_taps, gate_rows, up_rows, down_rows = weight_grads
    return (in_grad, grad_gate, grad_up, grad_down, grad_taps, gate_rows, up_rows, down_rows)


LANES = 128
CW = 256
HALO = 16
MID_LAG = 3
OUT_LAG = 18
MESH_ID = pl.DeviceIdType.MESH


def layer_kernel(
    n_rep, n_fs,
    x_ref, wg_ref, wu_ref, taps_ref, wd_ref, og_ref,
    in_grad_ref, down_ref, gate_ref, up_ref, taps_out_ref, rows_gate_ref, rows_up_ref, rows_down_ref,
    xt, send_part, recv_part, h_all, g_all, u_all, part, from_out, from_in, tot,
    acc, ig_send, ig_recv, tap_all, tap_out, tap_in, tap_sum, rows, rows_tp, rows_fs,
    rs_send, rs_recv, ag_send, ag_recv, a_send, out_recv, in_recv, b_send, loc_sem, misc,
):
    tok, feat = x_ref.shape
    cw = CW
    chunks = wg_ref.shape[1] // cw
    subs = feat // cw
    own_rows = tok // 2
    span = own_rows + HALO
    total_pieces = chunks * 3 * subs
    f32, bf16 = jnp.float32, jnp.bfloat16
    r = lax.axis_index("rep")
    f = lax.axis_index("fs")
    t = lax.axis_index("tp")
    half_rep = n_rep // 2
    is_left = r < half_rep
    toward = jnp.where(is_left, r + 1, r - 1)
    outward = jnp.where(is_left, r - 1, r + 1)
    is_end = jnp.logical_or(r == 0, r == n_rep - 1)
    not_end = jnp.logical_not(is_end)
    is_mid = jnp.logical_or(r == half_rep - 1, r == half_rep)
    not_mid = jnp.logical_not(is_mid)
    beside = f + 1 - 2 * lax.rem(f, 2)
    across = lax.rem(f + 2, 4)
    corner = lax.rem(beside + 2, 4)
    peers = [beside, across, corner]
    side = lax.rem(f, 2)
    top = f // 2
    own_cols = pl.ds(pl.multiple_of(side * LANES, LANES), LANES)
    own_toks = pl.ds(pl.multiple_of(top * own_rows, own_rows), own_rows)

    barrier = pltpu.get_barrier_semaphore()
    for k in range(n_fs - 1):
        pl.semaphore_signal(barrier, inc=1, device_id={"fs": peers[k]}, device_id_type=MESH_ID)
    pl.semaphore_signal(barrier, inc=1, device_id={"tp": 1 - t}, device_id_type=MESH_ID)
    pl.semaphore_signal(barrier, inc=1, device_id={"rep": toward}, device_id_type=MESH_ID)

    @pl.when(not_end)
    def _():
        pl.semaphore_signal(barrier, inc=1, device_id={"rep": outward}, device_id_type=MESH_ID)

    pl.semaphore_wait(barrier, n_fs + 1 + jnp.where(not_end, 1, 0))

    def remote(src, dst, send, recv, device):
        return pltpu.make_async_remote_copy(
            src_ref=src, dst_ref=dst, send_sem=send, recv_sem=recv,
            device_id=device, device_id_type=MESH_ID,
        )

    sent = []

    def rs_copy(c, tensor, k):
        s = (c * 3 + tensor) * (n_fs - 1) + k
        return remote(
            send_part.at[c, tensor, peers[k]], recv_part.at[c, tensor, k],
            rs_send.at[s], rs_recv.at[s], {"fs": peers[k]},
        )

    def reduce_start(c):
        cols = slice(c * cw, (c + 1) * cw)
        for tensor in range(3):
            if tensor == 0:
                value = jnp.dot(x_ref[...], wg_ref[:, cols], preferred_element_type=f32)
            elif tensor == 1:
                value = jnp.dot(x_ref[...], wu_ref[:, cols], preferred_element_type=f32)
            else:
                value = contract(og_ref[...], wd_ref[cols, :], 1, 1)
            value = value.astype(bf16)
            for g in range(n_fs):
                first = (g // 2) * (own_rows - HALO)
                lane = (g % 2) * LANES
                send_part[c, tensor, g] = value[first : first + span, lane : lane + LANES]
            for k in range(n_fs - 1):
                copy = rs_copy(c, tensor, k)
                copy.start()
                sent.append(copy)

    def reduced(c, tensor):
        value = send_part[c, tensor, f].astype(f32)
        for k in range(n_fs - 1):
            rs_copy(c, tensor, k).wait_recv()
            value = value + recv_part[c, tensor, k].astype(f32)
        return value.astype(bf16).astype(f32)

    def block(c, tensor, owner, part_of=None):
        col = lax.rem(owner, 2) * LANES
        row = (owner // 2) * own_rows
        if tensor == 0:
            size = LANES if part_of is None else LANES // 2
            start = col + (0 if part_of is None else part_of * size)
            return h_all.at[
                c, pl.ds(pl.multiple_of(start, size), size), pl.ds(pl.multiple_of(row, own_rows), own_rows)
            ]
        size = own_rows if part_of is None else own_rows // 2
        start = row + (0 if part_of is None else part_of * size)
        ref = g_all if tensor == 1 else u_all
        return ref.at[c, pl.ds(pl.multiple_of(start, size), size), pl.ds(pl.multiple_of(col, LANES), LANES)]

    def ag_copy(c, tensor, step, owner):
        s = (c * 3 + tensor) * 4
        if step == 0:
            ref, slot, target = block(c, tensor, owner), 0, beside
        elif step == 1:
            ref, slot, target = block(c, tensor, owner), 1, across
        elif step == 2:
            ref, slot, target = block(c, tensor, owner, 1), 2, beside
        else:
            ref, slot, target = block(c, tensor, owner, 0), 3, across
        return remote(ref, ref, ag_send.at[s + slot], ag_recv.at[s + slot], {"fs": target})

    def gather_start(c, tensor):
        for step in (0, 1):
            copy = ag_copy(c, tensor, step, f)
            copy.start()
            sent.append(copy)

    def forward(c, tensor):
        ag_copy(c, tensor, 0, beside).wait_recv()
        copy = ag_copy(c, tensor, 3, beside)
        copy.start()
        sent.append(copy)
        ag_copy(c, tensor, 1, across).wait_recv()
        copy = ag_copy(c, tensor, 2, across)
        copy.start()
        sent.append(copy)

    def gathered(c, tensor):
        ag_copy(c, tensor, 2, corner).wait_recv()
        ag_copy(c, tensor, 3, corner).wait_recv()

    def own(value):
        return jnp.where(top == 0, value[:own_rows], value[HALO:])

    row_ids = lax.broadcasted_iota(jnp.int32, (span, LANES), 0)

    def down(value, lag):
        if lag == 0:
            return value
        return jnp.where(row_ids >= lag, pltpu.roll(value, lag, 0), 0.0)

    def up(value, lag):
        if lag == 0:
            return value
        return jnp.where(row_ids < span - lag, pltpu.roll(value, span - lag, 0), 0.0)

    def elementwise(c):
        cols = pl.ds(pl.multiple_of(c * cw + side * LANES, LANES), LANES)
        weights = taps_ref[:, cols].astype(f32)
        gate = reduced(c, 0)
        pre = weights[0:1] * down(gate, KW - 1)
        for j in range(1, KW):
            pre = pre + weights[j : j + 1] * down(gate, KW - 1 - j)
        sig = 1.0 / (1.0 + jnp.exp(-pre))
        silu = pre * sig
        up_val = reduced(c, 1)
        h_all[c, own_cols, own_toks] = own(silu * up_val).T.astype(bf16)
        gather_start(c, 0)
        act = reduced(c, 2)
        pre_grad = act * up_val * sig * (1.0 + pre * (1.0 - sig))
        grad = weights[0:1] * up(pre_grad, KW - 1)
        for j in range(1, KW):
            grad = grad + weights[j : j + 1] * up(pre_grad, KW - 1 - j)
        g_all[c, own_toks, own_cols] = own(grad).astype(bf16)
        gather_start(c, 1)
        u_all[c, own_toks, own_cols] = own(act * silu).astype(bf16)
        gather_start(c, 2)
        for j in range(KW):
            tap_all[f, c * KW + j : c * KW + j + 1, :] = jnp.sum(
                own(down(gate, KW - 1 - j) * pre_grad), axis=0, keepdims=True
            )

    def part_copy(p):
        return remote(part.at[p], from_out.at[p], a_send.at[p], out_recv.at[p], {"rep": toward})

    def exchange_copy(p):
        return remote(part.at[p], from_in.at[p], a_send.at[p], in_recv.at[p], {"rep": toward})

    def total_copy(p, src):
        return remote(src.at[p], from_in.at[p], b_send.at[p], in_recv.at[p], {"rep": outward})

    def local_copy(p, src, tensor, wait):
        c = p // (3 * subs)
        q = p % subs
        along = pl.ds(pl.multiple_of(c * cw, cw), cw)
        inner = pl.ds(pl.multiple_of(q * cw, cw), cw)
        if tensor == 0:
            dst = down_ref.at[along, inner]
        elif tensor == 1:
            dst = gate_ref.at[inner, along]
        else:
            dst = up_ref.at[inner, along]
        copy = pltpu.make_async_copy(src.at[p], dst, loc_sem.at[p])
        if wait:
            copy.wait()
        else:
            copy.start()

    def store_out(p, src, wait=False):
        kind = (p // subs) % 3
        for tensor in range(3):
            @pl.when(kind == tensor)
            def _(tensor=tensor):
                local_copy(p, src, tensor, wait)

    def stage_a(p, value):
        @pl.when(not_end)
        def _():
            part_copy(p).wait_recv()
            part[p] = (value + from_out[p].astype(f32)).astype(bf16)

        @pl.when(is_end)
        def _():
            part[p] = value.astype(bf16)

        @pl.when(is_mid)
        def _():
            exchange_copy(p).start()

        @pl.when(not_mid)
        def _():
            part_copy(p).start()

    def norms(p, value):
        square = value * value
        lanes = square[:, :LANES]
        for g in range(1, square.shape[1] // LANES):
            lanes = lanes + square[:, g * LANES : (g + 1) * LANES]
        for i in range(cw // LANES):
            rows[pl.ds(p * (cw // LANES) + i, 1), :] = jnp.sum(
                lanes[i * LANES : (i + 1) * LANES].T, axis=0, keepdims=True
            )

    def stage_b_mid(p):
        exchange_copy(p).wait_recv()
        value = (part[p].astype(f32) + from_in[p].astype(f32)).astype(bf16)
        tot[p] = value

        @pl.when(not_end)
        def _():
            total_copy(p, tot).start()

        store_out(p, tot)
        norms(p, value.astype(f32))

    def stage_b_out(p):
        exchange_copy(p).wait_recv()

        @pl.when(not_end)
        def _():
            total_copy(p, from_in).start()

        store_out(p, from_in)
        norms(p, from_in[p].astype(f32))

    def stage_b(slot):
        @pl.when(jnp.logical_and(is_mid, jnp.logical_and(slot >= MID_LAG, slot < total_pieces + MID_LAG)))
        def _():
            stage_b_mid(slot - MID_LAG)

        @pl.when(jnp.logical_and(not_mid, slot >= OUT_LAG))
        def _():
            stage_b_out(slot - OUT_LAG)

    def segment(c, tensor):
        gathered(c, tensor)

        @pl.loop(0, subs)
        def _(q):
            p = (c * 3 + tensor) * subs + q
            if tensor == 0:
                value = jnp.dot(
                    h_all[c], og_ref[:, pl.ds(pl.multiple_of(q * cw, cw), cw)], preferred_element_type=f32
                )
            elif tensor == 1:
                value = jnp.dot(xt[q], g_all[c], preferred_element_type=f32)
            else:
                value = jnp.dot(xt[q], u_all[c], preferred_element_type=f32)
            stage_a(p, value)
            stage_b(p)

    def input_term(c):
        cols = slice(c * cw, (c + 1) * cw)
        term = contract(g_all[c], wg_ref[:, cols], 1, 1) + contract(u_all[c], wu_ref[:, cols], 1, 1)
        if c == 0:
            acc[...] = term
        else:
            acc[...] += term

    reduce_start(0)
    for q in range(subs):
        xt[q] = x_ref[:, q * cw : (q + 1) * cw].astype(f32).T.astype(bf16)
    elementwise(0)
    if chunks > 1:
        reduce_start(1)
    tap_peers = []

    def advance(c):
        if c < chunks:
            elementwise(c)
            if c + 1 < chunks:
                reduce_start(c + 1)
        else:
            for k in range(n_fs - 1):
                copy = remote(
                    tap_all.at[f], tap_all.at[f], misc.at[2 * k], misc.at[2 * k + 1], {"fs": peers[k]}
                )
                copy.start()
                tap_peers.append(copy)

    forward(0, 0)
    for c in range(chunks):
        if c > 0:
            advance(c + 1)
        segment(c, 0)
        if c == 0:
            forward(c, 1)
        segment(c, 1)
        if c == 0:
            forward(c, 2)
            advance(c + 1)
        segment(c, 2)
        if c + 1 < chunks:
            for tensor in range(3):
                forward(c + 1, tensor)
        input_term(c)

    m = 2 * (n_fs - 1)
    half = tok // 2
    ig_send[...] = acc[...].astype(bf16)
    ig_copy = remote(
        ig_send.at[pl.ds(pl.multiple_of((1 - t) * half, half), half)], ig_recv,
        misc.at[m], misc.at[m + 1], {"tp": 1 - t},
    )
    ig_copy.start()

    for copy in tap_peers:
        copy.wait()
    tap_part = remote(tap_all, tap_out, misc.at[m + 2], misc.at[m + 3], {"rep": toward})
    tap_exchange = remote(tap_all, tap_in, misc.at[m + 2], misc.at[m + 4], {"rep": toward})
    tap_total = remote(tap_sum, tap_in, misc.at[m + 5], misc.at[m + 4], {"rep": outward})

    @pl.when(not_end)
    def _():
        tap_part.wait_recv()
        tap_all[...] = tap_all[...] + tap_out[...]

    @pl.when(is_mid)
    def _():
        tap_exchange.start()

    @pl.when(not_mid)
    def _():
        tap_part.start()

    ig_copy.wait()
    in_grad_ref[...] = (
        ig_send[pl.ds(pl.multiple_of(t * half, half), half), :].astype(f32) + ig_recv[...].astype(f32)
    ).astype(bf16)

    @pl.loop(total_pieces, total_pieces + OUT_LAG)
    def _(slot):
        stage_b(slot)

    tap_exchange.wait_recv()

    @pl.when(is_mid)
    def _():
        tap_sum[...] = tap_all[...] + tap_in[...]

    @pl.when(not_mid)
    def _():
        tap_sum[...] = tap_in[...]

    @pl.when(not_end)
    def _():
        tap_total.start()

    rows_copies = [
        remote(rows, rows_tp, misc.at[m + 6], misc.at[m + 7], {"tp": 1 - t})
    ]
    for k in range(n_fs - 1):
        rows_copies.append(
            remote(rows, rows_fs.at[k], misc.at[m + 8 + 2 * k], misc.at[m + 9 + 2 * k], {"fs": peers[k]})
        )
    for copy in rows_copies:
        copy.start()

    for copy in sent:
        copy.wait_send()
    tap_part.wait_send()

    @pl.loop(0, total_pieces)
    def _(p):
        part_copy(p).wait_send()

        @pl.when(not_end)
        def _():
            total_copy(p, tot).wait_send()

        store_out(p, tot, True)

    for copy in rows_copies:
        copy.wait()
    per = cw // LANES
    for tensor, rows_ref in ((1, rows_gate_ref), (2, rows_up_ref)):
        for q in range(subs):
            for i in range(per):
                value = jnp.zeros((1, LANES), f32)
                for c in range(chunks):
                    at = ((c * 3 + tensor) * subs + q) * per + i
                    value = value + (rows[at : at + 1, :] + rows_tp[at : at + 1, :])
                lane = (q * per + i) * LANES
                rows_ref[:, lane : lane + LANES] = value
    for c in range(chunks):
        for i in range(per):
            value = jnp.zeros((1, LANES), f32)
            for q in range(subs):
                at = (c * 3 * subs + q) * per + i
                value = value + rows[at : at + 1, :]
                for k in range(n_fs - 1):
                    value = value + rows_fs[k, at : at + 1, :]
            lane = (c * per + i) * LANES
            rows_down_ref[:, lane : lane + LANES] = value
            for j in range(KW):
                at = c * KW + j
                taps_out_ref[j : j + 1, lane : lane + LANES] = (
                    tap_sum[i, at : at + 1, :] + tap_sum[i + 2, at : at + 1, :]
                )

    @pl.when(not_end)
    def _():
        tap_total.wait_send()


def fits(shape, inputs, w_gate):
    n_rep, n_fs, n_tp = shape["rep"], shape["fs"], shape["tp"]
    tok, feat = inputs.shape
    return (
        n_rep == 4 and n_fs == 4 and n_tp == 2 and feat == 2 * CW
        and w_gate.shape[1] % CW == 0 and w_gate.shape[1] <= 1536 and tok % LANES == 0 and tok <= 512
    )


def fused_shards(shape, inputs, w_gate, w_up, conv_taps, w_down, out_grad):
    if not fits(shape, inputs, w_gate):
        return shards(inputs, w_gate, w_up, conv_taps, w_down, out_grad)
    n_rep, n_fs = shape["rep"], shape["fs"]
    tok, feat = inputs.shape
    hid = w_gate.shape[1]
    cw = CW
    chunks = hid // cw
    subs = feat // cw
    pieces = chunks * 3 * subs
    bf16, f32 = jnp.bfloat16, jnp.float32
    vmem = pl.BlockSpec(memory_space=pltpu.VMEM)
    hops = chunks * 3 * (n_fs - 1)
    dma = pltpu.SemaphoreType.DMA
    in_grad, down, gate, up, taps, rows_gate, rows_up, rows_down = pl.pallas_call(
        functools.partial(layer_kernel, n_rep, n_fs),
        out_shape=(
            jax.ShapeDtypeStruct((tok // 2, feat), bf16),
            jax.ShapeDtypeStruct((hid, feat), bf16),
            jax.ShapeDtypeStruct((feat, hid), bf16),
            jax.ShapeDtypeStruct((feat, hid), bf16),
            jax.ShapeDtypeStruct((KW, hid), f32),
            jax.ShapeDtypeStruct((1, feat), f32),
            jax.ShapeDtypeStruct((1, feat), f32),
            jax.ShapeDtypeStruct((1, hid), f32),
        ),
        in_specs=[vmem] * 6,
        out_specs=(vmem,) + (pl.BlockSpec(memory_space=pl.ANY),) * 3 + (vmem,) * 4,
        scratch_shapes=[
            pltpu.VMEM((subs, cw, tok), bf16),
            pltpu.VMEM((chunks, 3, n_fs, tok // 2 + HALO, LANES), bf16),
            pltpu.VMEM((chunks, 3, n_fs - 1, tok // 2 + HALO, LANES), bf16),
            pltpu.VMEM((chunks, cw, tok), bf16),
            pltpu.VMEM((chunks, tok, cw), bf16),
            pltpu.VMEM((chunks, tok, cw), bf16),
            pltpu.VMEM((pieces, cw, cw), bf16),
            pltpu.VMEM((pieces, cw, cw), bf16),
            pltpu.VMEM((pieces, cw, cw), bf16),
            pltpu.VMEM((pieces, cw, cw), bf16),
            pltpu.VMEM((tok, feat), f32),
            pltpu.VMEM((tok, feat), bf16),
            pltpu.VMEM((tok // 2, feat), bf16),
            pltpu.VMEM((n_fs, chunks * KW, LANES), f32),
            pltpu.VMEM((n_fs, chunks * KW, LANES), f32),
            pltpu.VMEM((n_fs, chunks * KW, LANES), f32),
            pltpu.VMEM((n_fs, chunks * KW, LANES), f32),
            pltpu.VMEM((2 * pieces, LANES), f32),
            pltpu.VMEM((2 * pieces, LANES), f32),
            pltpu.VMEM((n_fs - 1, 2 * pieces, LANES), f32),
            dma((hops,)), dma((hops,)), dma((chunks * 12,)), dma((chunks * 12,)),
            dma((pieces,)), dma((pieces,)), dma((pieces,)), dma((pieces,)), dma((pieces,)),
            dma((4 * (n_fs - 1) + 8,)),
        ],
        compiler_params=pltpu.CompilerParams(
            collective_id=0, has_side_effects=True, vmem_limit_bytes=60 * 1024 * 1024
        ),
    )(inputs, w_gate, w_up, conv_taps, w_down, out_grad)
    return (
        in_grad, gate.astype(f32), up.astype(f32), down.astype(f32), taps,
        rows_gate.reshape(feat), rows_up.reshape(feat), rows_down.reshape(hid),
    )


def solution(mesh):
    return jax.shard_map(
        functools.partial(fused_shards, dict(mesh.shape)),
        mesh=mesh,
        in_specs=(
            P("rep", "fs"),
            P("fs", "tp"),
            P("fs", "tp"),
            P(None, "tp"),
            P("tp", "fs"),
            P("rep", "fs"),
        ),
        out_specs=(
            P(("rep", "tp"), "fs"),
            P("fs", "tp"),
            P("fs", "tp"),
            P("tp", "fs"),
            P(None, "tp"),
            P("fs"),
            P("fs"),
            P("tp"),
        ),
        check_vma=False,
    )
```
